32 devices in a mesh: gr: 2 (over x), fs: 4 (over z), tp: 4 (over y, core).
Axes of the slice: x: 2, y: 2, z: 4, core: 2. Of those that a mesh axis runs over, the one named last changes fastest.
Arguments:
- prompt_tokens: bfloat16 [4096, 2048], P(('gr', 'fs', 'tp')), may hold values from -60 to 60
- norm_gain: float32 [2048], P(('gr', 'fs')), may hold values from 0.1 to 1.9
- up_master: float32 [2048, 8192], P(('gr', 'fs'), 'tp'), may hold values from -0.125 to 0.125
- down_master: float32 [2048, 8192], P(('gr', 'fs'), 'tp'), may hold values from -0.0625 to 0.0625
Outputs:
- up_served: bfloat16 [2048, 8192], P(None, 'tp')
- down_served: bfloat16 [2048, 8192], P(None, 'tp')
- mlp_output: bfloat16 [4096, 2048], P(('gr', 'fs', 'tp'))
The draws below stay inside these ranges and needn't reach their ends.
All inputs are finite; a program needn't handle non-finite values.
Results may differ from the reference program's by a relative error of at most 0.014.
Values may be sent and summed in bfloat16 or wider, within the bound.
No kernel may reach another device: no remote copies, remote signals or barrier semaphores. Data moves between devices by JAX's collectives and lax.ppermute only.
A program may use at most 128 MiB of HBM per device.

```python
import math
import jax
import jax.numpy as jnp
from jax import lax

D = 2048
FF = 8192
TOKENS = 4096
N_TP = 4


def draw_prompt_tokens(key, part):
    entry_key, scale_key = jax.random.split(jax.random.fold_in(key, 17))
    entries = jnp.clip(jax.random.normal(entry_key, (TOKENS, D), jnp.float32), -5.0, 5.0)
    scales = jnp.exp(jax.random.uniform(scale_key, (TOKENS,), jnp.float32, 0.0, jnp.log(10.0)))
    return (entries * scales[:, None]).astype(jnp.bfloat16)


def level_of(key, dims, pieces, least, high):
    def one(axis_at, parts):
        steps = jax.random.uniform(jax.random.fold_in(jax.random.fold_in(key, 6), axis_at), (parts,), jnp.float32, least / len(pieces), high / len(pieces))
        return jnp.repeat(jnp.exp(steps), dims[axis_at] // parts).reshape((-1,) + (1,) * (len(dims) - axis_at - 1))

    level = one(*pieces[0])
    for cut in pieces[1:]:
        level = level * one(*cut)
    return level


def bell_draw(key, dims, spread, reach, shards=(), held_as=jnp.bfloat16):
    result = jax.random.normal(key, dims, jnp.float32) * spread
    if len(shards) > 0:
        result = level_of(key, dims, shards, -0.22, 0.18) * result
    return jnp.clip(result, min=-reach, max=reach).astype(held_as)


def setup_inputs(seed: int = 0) -> dict:
    seeds = jax.random.split(jax.random.key(seed), 5)
    prompt_tokens = draw_prompt_tokens(jax.random.fold_in(seeds[4], 71), 0)
    norm_gain = jnp.clip(1.0 + 0.18 * jax.random.normal(seeds[1], (D,), jnp.float32), 0.1, 1.9)
    up_master = bell_draw(seeds[2], (D, FF), D ** -0.5, 0.125, ((0, 8), (1, 4)), jnp.float32)
    down_master = bell_draw(seeds[3], (D, FF), FF ** -0.5, 0.0625, ((0, 8), (1, 4)), jnp.float32)
    return {"prompt_tokens": prompt_tokens, "norm_gain": norm_gain, "up_master": up_master, "down_master": down_master}


def reference(prompt_tokens, norm_gain, up_master, down_master):
    up_served = (up_master * norm_gain[:, None]).astype(jnp.bfloat16)
    down_served = down_master.astype(jnp.bfloat16)
    floats = prompt_tokens.astype(jnp.float32)
    mean_square = lax.optimization_barrier(lax.optimization_barrier(jnp.mean(floats * floats, axis=1, keepdims=True)))
    normed = (floats * lax.rsqrt(mean_square + 1e-06)).astype(jnp.bfloat16)
    block = math.gcd(TOKENS, 1024)
    width = FF // N_TP
    down_blocks = down_served.reshape(D, N_TP, width).astype(jnp.float32)

    def one_block(rows):
        pre = jnp.dot(rows, up_served, preferred_element_type=jnp.float32)
        hidden = jnp.square(jnp.maximum(pre, 0.0)).astype(jnp.bfloat16)
        split = hidden.reshape(block, N_TP, width).astype(jnp.float32)
        partial_value = jnp.einsum('rkf,dkf->krd', split, down_blocks).astype(jnp.bfloat16)
        partial_value = lax.optimization_barrier(partial_value)
        return lax.optimization_barrier(jnp.sum(partial_value.astype(jnp.float32), axis=0)).astype(jnp.bfloat16)
    outputs = lax.map(one_block, normed.reshape(TOKENS // block, block, D))
    return (up_served, down_served, outputs.reshape(TOKENS, D))
```

```python
import jax
import jax.numpy as jnp
import numpy as np
from jax import lax
from jax.sharding import PartitionSpec as P

RING = ("gr", "fs")


def ring_order(groups, members):
    order = []
    for g in range(groups):
        line = range(members) if g % 2 == 0 else range(members - 1, -1, -1)
        order += [g * members + f for f in line]
    return order


def on_device(mesh):
    order = ring_order(mesh.shape["gr"], mesh.shape["fs"])
    size, n_tp = len(order), mesh.shape["tp"]
    forward = [(order[i], order[(i + 1) % size]) for i in range(size)]
    backward = [(b, a) for a, b in forward]
    place = {device: i for i, device in enumerate(order)}
    owner_at = np.array(
        [[order[(place[d] - hop) % size] for hop in range(size)] for d in range(size)], np.int32
    )
    if n_tp & (n_tp - 1) == 0:
        to_peer = [[(t, t ^ k) for t in range(n_tp)] for k in range(1, n_tp)]
        from_peer = to_peer
    else:
        to_peer = [[(t, (t + k) % n_tp) for t in range(n_tp)] for k in range(1, n_tp)]
        from_peer = [[(b, a) for a, b in pairs] for pairs in to_peer]
    last = size // 2

    def body(prompt_tokens, norm_gain, up_master, down_master):
        owners = lax.dynamic_slice(
            jnp.asarray(owner_at), (lax.axis_index(RING), 0), (1, size)
        ).reshape(size)
        rows, width = up_master.shape
        half = rows // 2

        def travel(shard):
            halves = [shard[:half], shard[half:]]
            cw, ccw = list(halves), list(halves)
            arrived = [[(0, 0, halves[0]), (0, 1, halves[1])]]
            for hop in range(1, last + 1):
                got = []
                for first in (0, 1):
                    for runs, pairs, sign, s in ((cw, forward, 1, first), (ccw, backward, -1, 1 - first)):
                        if size % 2 == 0 and hop == last and first == 1:
                            continue
                        runs[s] = lax.ppermute(runs[s], RING, pairs)
                        got.append(((sign * hop) % size, s, runs[s]))
                arrived.append(got)
            return arrived

        def collect(arrived):
            whole = jnp.zeros((rows * size, width), jnp.bfloat16)
            for got in arrived:
                for hop, s, part in got:
                    whole = lax.dynamic_update_slice(whole, part, (owners[hop] * rows + s * half, 0))
            return whole

        up_parts = travel((up_master * norm_gain[:, None]).astype(jnp.bfloat16))
        down_parts = travel(down_master.astype(jnp.bfloat16))

        floats = prompt_tokens.astype(jnp.float32)
        mean_square = jnp.mean(floats * floats, axis=1, keepdims=True)
        normed = (floats * lax.rsqrt(mean_square + 1e-06)).astype(jnp.bfloat16)
        tokens = normed.shape[0]
        normed_all = jnp.concatenate(
            [normed] + [lax.ppermute(normed, "tp", pairs) for pairs in from_peer]
        )

        up_served = collect(up_parts)
        down_served = collect(down_parts)
        pre = jnp.dot(normed_all, up_served, preferred_element_type=jnp.float32)
        hidden = jnp.square(jnp.maximum(pre, 0.0)).astype(jnp.bfloat16)

        n_early = max(1, last - 2)
        groups = [
            sum(down_parts[: n_early + 1], []),
            *[got for got in down_parts[n_early + 1 :]],
        ]
        out = jnp.zeros((tokens, rows * size), jnp.bfloat16)
        for group in groups:
            partial = jnp.concatenate(
                [
                    lax.dot_general(
                        hidden, part, (((1,), (1,)), ((), ())), preferred_element_type=jnp.float32
                    ).astype(jnp.bfloat16)
                    for _, _, part in group
                ],
                axis=1,
            )
            total = partial[:tokens].astype(jnp.float32)
            for k, pairs in enumerate(to_peer, 1):
                block = partial[k * tokens : (k + 1) * tokens]
                total += lax.ppermute(block, "tp", pairs).astype(jnp.float32)
            total = total.astype(jnp.bfloat16)
            for i, (hop, s, _) in enumerate(group):
                out = lax.dynamic_update_slice(
                    out, total[:, i * half : (i + 1) * half], (0, owners[hop] * rows + s * half)
                )
        return up_served, down_served, out

    return body


def solution(mesh):
    placed = (
        P(("gr", "fs", "tp"), None),
        P(("gr", "fs")),
        P(("gr", "fs"), "tp"),
        P(("gr", "fs"), "tp"),
    )
    return jax.shard_map(
        on_device(mesh),
        mesh=mesh,
        in_specs=placed,
        out_specs=(P(None, "tp"), P(None, "tp"), P(("gr", "fs", "tp"), None)),
        check_vma=False,
    )
```
